32 devices in a mesh: ep: 16 (over z, y, core), tp: 2 (over x).
Axes of the slice: x: 2, y: 2, z: 4, core: 2. Of those that a mesh axis runs over, the one named last changes fastest.
Arguments:
- tokens: bfloat16 [2048, 2048], P('ep'), may hold values from -6 to 6
- expert_ids: int32 [2048, 2], P('ep'), may hold values from 0 to 15, as said below
- route_weights: bfloat16 [2048, 2], P('ep'), may hold values from 0.099609375 to 1
- cotangent: bfloat16 [2048, 2048], P('ep'), may hold values from -3 to 3
- w_gate: bfloat16 [16, 2048, 512], P('ep', None, 'tp'), may hold values from -0.125 to 0.125
- w_up: bfloat16 [16, 2048, 512], P('ep', None, 'tp'), may hold values from -0.125 to 0.125
- w_down: bfloat16 [16, 512, 2048], P('ep', 'tp'), may hold values from -0.25 to 0.25
Outputs:
- token_grad: bfloat16 [2048, 2048], P('ep', 'tp')
- route_grad: bfloat16 [2048, 2], P('ep')
- grad_gate: bfloat16 [16, 2048, 512], P('ep', None, 'tp')
- grad_up: bfloat16 [16, 2048, 512], P('ep', None, 'tp')
- grad_down: bfloat16 [16, 512, 2048], P('ep', 'tp')
- gate_rows: float32 [16, 2048], P('ep')
- up_rows: float32 [16, 2048], P('ep')
- down_rows: float32 [16, 512], P('ep', 'tp')
The draws below stay inside these ranges and needn't reach their ends.
Inputs may be any that keep to these rules, and one draw needn't show every extreme that they name: `expert_ids`: each row names 2 different experts of one group: both lie in g * 4 to (g + 1) * 4 - 1 for the row's group g. In the rows of one device (aligned blocks of 128 rows) no expert is named more than 32 times, and in every block some expert is named exactly 32 times.
All inputs are finite; a program needn't handle non-finite values.
Results may differ from the reference program's by a relative error of at most 0.012.
Values may be sent and summed in bfloat16 or wider, within the bound.
No kernel may reach another device: no remote copies, remote signals or barrier semaphores. Data moves between devices by JAX's collectives and lax.ppermute only.
A program may use at most 64 MiB of HBM per device.

```python
import jax
import jax.numpy as jnp
from jax import lax

D = 2048
F = 512
GROUPS = 4
TOPK = 2
TOK_DEV = 128
EXPERTS = 16
CAP = 32
TOKENS = 2048
N_EP = 16
N_TP = 2


def draw_expert_ids(key, part):
    per_group = EXPERTS // GROUPS
    blocks = TOKENS // TOK_DEV
    hot_group = jax.random.randint(jax.random.fold_in(key, 11), (), 0, GROUPS)
    hot_member = jax.random.randint(jax.random.fold_in(key, 12), (), 0, per_group)
    block_keys = jax.random.split(jax.random.fold_in(key, 13), blocks)
    group_ids = jnp.arange(GROUPS, dtype=jnp.int32)
    member_ids = jnp.arange(per_group, dtype=jnp.int32)

    def one_block(block_key):
        key_a, key_b, key_c, key_d, key_e = jax.random.split(block_key, 5)
        hot_size = jax.random.randint(key_a, (), max(CAP, TOK_DEV // 4), TOK_DEV // 2 + 1)
        remain = TOK_DEV - hot_size
        third = remain // 3
        jitter = remain // 8
        first_size = jax.random.randint(key_b, (), third - jitter, third + jitter + 1)
        second_size = jax.random.randint(key_c, (), third - jitter, third + jitter + 1)
        others = jnp.stack([first_size, second_size, remain - first_size - second_size])
        other_slot = jnp.minimum((group_ids - hot_group - 1) % GROUPS, 2)
        sizes = jnp.where(group_ids == hot_group, hot_size, others[other_slot]).astype(jnp.int32)
        ends = jnp.cumsum(sizes)
        starts = ends - sizes
        fill_step = jnp.maximum(jnp.minimum(CAP, sizes), 1)
        ranks = jax.random.permutation(key_d, TOK_DEV).astype(jnp.int32)
        member_group = jnp.sum((ranks[:, None] >= ends[None, :]).astype(jnp.int32), axis=1)
        inner = ranks - starts[member_group]
        count = sizes[member_group]
        stride = fill_step[member_group]
        scores = jax.random.randint(key_e, (GROUPS, per_group), 0, 1 << 20) * per_group + member_ids[None, :]
        pinned = (group_ids[:, None] == hot_group) & (member_ids[None, :] == hot_member)
        scores = jnp.where(pinned, -1, scores)
        ordering = jnp.argsort(scores, axis=1).astype(jnp.int32)
        first_pick = ordering[member_group, inner // stride]
        second_pick = ordering[member_group, (inner + count) // stride]
        base_ids = member_group * per_group
        return jnp.stack([base_ids + first_pick, base_ids + second_pick], axis=1)
    return jax.vmap(one_block)(block_keys).reshape(TOKENS, TOPK).astype(jnp.int32)


def block_levels(key, extent, pieces, least, largest):
    loudness = 1.0
    for position, parts in pieces:
        steps = jax.random.uniform(jax.random.fold_in(jax.random.fold_in(key, 6), position), (parts,), jnp.float32, least / len(pieces), largest / len(pieces))
        loudness = loudness * jnp.repeat(jnp.exp(steps), extent[position] // parts).reshape((-1,) + (1,) * (len(extent) - 1 - position))
    return loudness


def noise(rng, shape, spread, bound, cuts=(), kind=jnp.bfloat16):
    result = jax.random.normal(rng, shape, jnp.float32) * spread
    if len(cuts) > 0:
        result = block_levels(rng, shape, cuts, -0.22, 0.18) * result
    return jnp.clip(result, min=-bound, max=bound).astype(kind)


def setup_inputs(seed: int = 0) -> dict:
    streams_of = jax.random.split(jax.random.key(seed), 8)
    tokens = noise(streams_of[0], (TOKENS, D), 1.0, 6.0, ((0, 16),))
    expert_ids = draw_expert_ids(jax.random.fold_in(streams_of[7], 71), 0)
    route_weights = jnp.clip(0.099609375 + 0.9003906 * jax.random.uniform(streams_of[2], (TOKENS, TOPK), jnp.float32) ** block_levels(streams_of[2], (TOKENS, TOPK), ((0, 16),), -0.2, 0.2), 0.099609375, 1.0).astype(jnp.bfloat16)
    cotangent = noise(streams_of[3], (TOKENS, D), 0.5, 3.0, ((0, 16),))
    w_gate = noise(streams_of[4], (EXPERTS, D, F), D ** -0.5, 0.125, ((0, 16), (2, 2)))
    w_up = noise(streams_of[5], (EXPERTS, D, F), D ** -0.5, 0.125, ((0, 16), (2, 2)))
    w_down = noise(streams_of[6], (EXPERTS, F, D), F ** -0.5, 0.25, ((0, 16), (1, 2)))
    return {"tokens": tokens, "expert_ids": expert_ids, "route_weights": route_weights, "cotangent": cotangent, "w_gate": w_gate, "w_up": w_up, "w_down": w_down}


def reference(tokens, expert_ids, route_weights, cotangent, w_gate, w_up, w_down):
    assigns = TOKENS * TOPK
    slot_total = N_EP * CAP
    quarter = F // N_TP
    flat_ids = expert_ids.reshape(-1).astype(jnp.int32)
    weight_flat = jnp.concatenate([route_weights.reshape(-1).astype(jnp.float32), jnp.zeros((1,), jnp.float32)])
    rows_pad = jnp.concatenate([tokens, jnp.zeros((1, D), jnp.bfloat16)], axis=0)
    cot_pad = jnp.concatenate([cotangent, jnp.zeros((1, D), jnp.bfloat16)], axis=0)

    def per_expert(expert):
        picked = jnp.nonzero(flat_ids == expert, size=slot_total, fill_value=assigns)[0].astype(jnp.int32)
        holder = (picked // TOPK).astype(jnp.int32)
        slot_rows = rows_pad[holder]
        slot_cot = cot_pad[holder]
        slot_scale = weight_flat[picked]
        gate_cols = w_gate[expert]
        up_cols = w_up[expert]
        down_rows_w = w_down[expert]
        gate_pre = jnp.dot(slot_rows, gate_cols, preferred_element_type=jnp.float32)
        up_pre = jnp.dot(slot_rows, up_cols, preferred_element_type=jnp.float32)
        hidden_back = lax.dot_general(slot_cot, down_rows_w, (((1,), (1,)), ((), ())), preferred_element_type=jnp.float32)
        gate_sig = jax.nn.sigmoid(gate_pre)
        activated = gate_pre * gate_sig
        hidden = activated * up_pre
        route_sum = jnp.sum(hidden * hidden_back, axis=1)
        hidden_cot = slot_scale[:, None] * hidden_back
        up_cot = (hidden_cot * activated).astype(jnp.bfloat16)
        gate_cot = (hidden_cot * up_pre * gate_sig * (1.0 + gate_pre * (1.0 - gate_sig))).astype(jnp.bfloat16)
        weighted_hidden = (slot_scale[:, None] * hidden).astype(jnp.bfloat16)
        grad_down_e = lax.dot_general(weighted_hidden, slot_cot, (((0,), (0,)), ((), ())), preferred_element_type=jnp.float32).astype(jnp.bfloat16)
        grad_gate_e = lax.dot_general(slot_rows, gate_cot, (((0,), (0,)), ((), ())), preferred_element_type=jnp.float32).astype(jnp.bfloat16)
        grad_up_e = lax.dot_general(slot_rows, up_cot, (((0,), (0,)), ((), ())), preferred_element_type=jnp.float32).astype(jnp.bfloat16)
        gate_blocks = gate_cot.astype(jnp.float32).reshape(slot_total, N_TP, quarter)
        up_blocks = up_cot.astype(jnp.float32).reshape(slot_total, N_TP, quarter)
        gate_w_blocks = gate_cols.astype(jnp.float32).reshape(D, N_TP, quarter)
        up_w_blocks = up_cols.astype(jnp.float32).reshape(D, N_TP, quarter)
        block_part = jnp.einsum('sjf,djf->sjd', gate_blocks, gate_w_blocks, precision=lax.Precision.HIGHEST)
        block_part = block_part + jnp.einsum('sjf,djf->sjd', up_blocks, up_w_blocks, precision=lax.Precision.HIGHEST)
        block_round = lax.optimization_barrier(block_part.astype(jnp.bfloat16))
        pair_grad = jnp.sum(block_round.astype(jnp.float32), axis=1).astype(jnp.bfloat16)
        return grad_gate_e, grad_up_e, grad_down_e, pair_grad, route_sum.astype(jnp.bfloat16), picked

    grad_gate, grad_up, grad_down, pair_grad, route_part, picked = lax.map(per_expert, jnp.arange(EXPERTS, dtype=jnp.int32))
    index_all = picked.reshape(-1)
    token_acc = jnp.zeros((assigns + 1, D), jnp.float32).at[index_all].set(pair_grad.reshape(-1, D).astype(jnp.float32))
    token_grad = jnp.sum(token_acc[:assigns].reshape(TOKENS, TOPK, D), axis=1).astype(jnp.bfloat16)
    route_acc = jnp.zeros((assigns + 1,), jnp.bfloat16).at[index_all].set(route_part.reshape(-1))
    route_grad = route_acc[:assigns].reshape(TOKENS, TOPK)
    gate_rows = jnp.sum(jnp.square(grad_gate.astype(jnp.float32)), axis=2)
    up_rows = jnp.sum(jnp.square(grad_up.astype(jnp.float32)), axis=2)
    down_rows = jnp.sum(jnp.square(grad_down.astype(jnp.float32)), axis=2)
    return (token_grad, route_grad, grad_gate, grad_up, grad_down, gate_rows, up_rows, down_rows)
```

```python
import jax
import jax.numpy as jnp
from jax import lax
from jax.sharding import PartitionSpec as P

TOPK = 2


def on_device(tokens, expert_ids, route_weights, cotangent, w_gate, w_up, w_down):
    tok_rows, model_width = tokens.shape
    experts = lax.axis_size("ep")
    splits = lax.axis_size("tp")
    capacity = 2 * tok_rows * TOPK // experts
    slot_count = experts * capacity
    assigns = tok_rows * TOPK
    flat_ids = expert_ids.reshape(-1)
    onehot = (flat_ids[:, None] == jnp.arange(experts, dtype=jnp.int32)[None, :]).astype(
        jnp.float32
    )
    assign_order = jnp.arange(assigns, dtype=jnp.int32)
    earlier = (assign_order[:, None] > assign_order[None, :]).astype(jnp.float32)
    before = jnp.dot(earlier, onehot, precision=lax.Precision.HIGHEST)
    slot_rank = jnp.sum(before * onehot, axis=1).astype(jnp.int32)
    position = flat_ids * capacity + slot_rank
    slot_owner = jnp.full((slot_count,), tok_rows, jnp.int32).at[position].set(assign_order // TOPK)
    slot_scale = jnp.zeros((slot_count,), jnp.bfloat16).at[position].set(route_weights.reshape(-1))
    slice_width = model_width // splits
    slice_start = lax.axis_index("tp") * slice_width
    rows_slice = lax.dynamic_slice_in_dim(tokens, slice_start, slice_width, 1)
    cot_slice = lax.dynamic_slice_in_dim(cotangent, slice_start, slice_width, 1)
    rows_pad = jnp.concatenate([rows_slice, jnp.zeros((1, slice_width), jnp.bfloat16)], axis=0)
    cot_pad = jnp.concatenate([cot_slice, jnp.zeros((1, slice_width), jnp.bfloat16)], axis=0)
    outgoing = rows_pad[slot_owner]
    outgoing_cot = cot_pad[slot_owner]
    part_rows, part_cot, got_scale = (
        lax.all_to_all(outgoing, "ep", split_axis=0, concat_axis=0, tiled=True),
        lax.all_to_all(outgoing_cot, "ep", split_axis=0, concat_axis=0, tiled=True),
        lax.all_to_all(slot_scale, "ep", split_axis=0, concat_axis=0, tiled=True),
    )
    slot_rows, slot_cot = (
        lax.all_gather(part_rows, "tp", axis=1, tiled=True),
        lax.all_gather(part_cot, "tp", axis=1, tiled=True),
    )
    scale_col = got_scale.reshape(slot_count, 1).astype(jnp.float32)
    gate_cols = w_gate[0]
    up_cols = w_up[0]
    down_part = w_down[0]
    gate_pre = jnp.dot(slot_rows, gate_cols, preferred_element_type=jnp.float32)
    up_pre = jnp.dot(slot_rows, up_cols, preferred_element_type=jnp.float32)
    hidden_back = lax.dot_general(
        slot_cot, down_part, (((1,), (1,)), ((), ())), preferred_element_type=jnp.float32
    )
    gate_sig = jax.nn.sigmoid(gate_pre)
    activated = gate_pre * gate_sig
    hidden = activated * up_pre
    route_part = jnp.sum(hidden * hidden_back, axis=1)
    hidden_cot = scale_col * hidden_back
    up_cot = (hidden_cot * activated).astype(jnp.bfloat16)
    gate_cot = (hidden_cot * up_pre * gate_sig * (1.0 + gate_pre * (1.0 - gate_sig))).astype(
        jnp.bfloat16
    )
    weighted_hidden = (scale_col * hidden).astype(jnp.bfloat16)
    grad_down = lax.dot_general(
        weighted_hidden, slot_cot, (((0,), (0,)), ((), ())), preferred_element_type=jnp.float32
    ).astype(jnp.bfloat16)
    grad_gate = lax.dot_general(
        slot_rows, gate_cot, (((0,), (0,)), ((), ())), preferred_element_type=jnp.float32
    ).astype(jnp.bfloat16)
    grad_up = lax.dot_general(
        slot_rows, up_cot, (((0,), (0,)), ((), ())), preferred_element_type=jnp.float32
    ).astype(jnp.bfloat16)
    token_term = lax.dot_general(
        gate_cot, gate_cols, (((1,), (1,)), ((), ())), preferred_element_type=jnp.float32
    )
    token_term = token_term + lax.dot_general(
        up_cot, up_cols, (((1,), (1,)), ((), ())), preferred_element_type=jnp.float32
    )
    reduced = lax.psum_scatter(
        token_term.astype(jnp.bfloat16), "tp", scatter_dimension=1, tiled=True
    )
    gate_square = jnp.sum(jnp.square(grad_gate.astype(jnp.float32)), axis=1)
    up_square = jnp.sum(jnp.square(grad_up.astype(jnp.float32)), axis=1)
    down_square = jnp.sum(jnp.square(grad_down.astype(jnp.float32)), axis=1)
    route_total, gate_rows, up_rows = lax.psum((route_part, gate_square, up_square), "tp")
    back_rows, back_route = (
        lax.all_to_all(reduced, "ep", split_axis=0, concat_axis=0, tiled=True),
        lax.all_to_all(
            route_total.astype(jnp.bfloat16), "ep", split_axis=0, concat_axis=0, tiled=True
        ),
    )
    per_assign = back_rows[position].astype(jnp.float32).reshape(tok_rows, TOPK, -1)
    token_grad = jnp.sum(per_assign, axis=1).astype(jnp.bfloat16)
    route_grad = back_route[position].reshape(tok_rows, TOPK)
    return (
        token_grad,
        route_grad,
        grad_gate[None],
        grad_up[None],
        grad_down[None],
        gate_rows[None],
        up_rows[None],
        down_square[None],
    )

GROUPS = 4
LANES = 128


def flip(value, axis, bit):
    size = lax.axis_size(axis)
    return lax.ppermute(value, axis, [(i, i ^ bit) for i in range(size)])


def mm(a, b, dims):
    return lax.dot_general(a, b, (dims, ((), ())), preferred_element_type=jnp.float32)


def add(a, b):
    return (a.astype(jnp.float32) + b.astype(jnp.float32)).astype(jnp.bfloat16)


def in_groups(tokens, expert_ids, route_weights, cotangent, w_gate, w_up, w_down):
    tok_rows, width = tokens.shape
    experts = lax.axis_size("ep")
    splits = lax.axis_size("tp")
    members = experts // GROUPS
    cap = tok_rows * TOPK // GROUPS
    half = width // splits
    my_x = lax.axis_index("tp")
    my_ep = lax.axis_index("ep")
    my_group = my_ep // members
    my_member = my_ep % members
    core_bit, row_bit = 1, members // 2
    bf = jnp.bfloat16

    group = (expert_ids[:, 0] // members) ^ my_group
    member = expert_ids % members
    onehot = (group[:, None] == jnp.arange(GROUPS, dtype=jnp.int32)[None, :]).astype(bf)
    order = jnp.arange(tok_rows, dtype=jnp.int32)
    earlier = (order[:, None] > order[None, :]).astype(bf)
    before = mm(earlier, onehot, ((1,), (0,)))
    rank = jnp.sum(before * onehot.astype(jnp.float32), axis=1).astype(jnp.int32)
    slot = group * cap + rank
    pack = (jnp.arange(GROUPS * cap, dtype=jnp.int32)[:, None] == slot[None, :]).astype(bf)
    lane = jnp.arange(LANES, dtype=jnp.int32)[None, :]
    picks = [lane == member[:, k : k + 1] for k in range(TOPK)]
    weights = sum(
        jnp.where(picks[k], route_weights[:, k : k + 1].astype(jnp.float32), 0.0)
        for k in range(TOPK)
    ).astype(bf)
    rows_half = lax.dynamic_slice_in_dim(tokens, my_x * half, half, 1)
    cot_half = lax.dynamic_slice_in_dim(cotangent, my_x * half, half, 1)
    rows_half = jnp.concatenate([rows_half, weights], axis=1)

    def to_group(source):
        got = []
        for k in range(GROUPS):
            piece = mm(pack[k * cap : (k + 1) * cap], source, ((1,), (0,))).astype(bf)
            got.append(piece if k == 0 else flip(piece, "ep", k * members))
        return jnp.concatenate(got, axis=0)

    def in_plane(own):
        cut = own.shape[0] // 2
        over_x = flip(own, "tp", 1)
        over_y = flip(own, "ep", row_bit)
        diag_a = flip(over_y[:cut, :half], "tp", 1)
        diag_b = flip(over_x[cut:, :half], "ep", row_bit)
        diag = jnp.concatenate([diag_a, diag_b], axis=0)
        mine = [own, over_y]
        other = [over_x[:, :half], diag]
        mine = mine + [flip(v, "ep", core_bit) for v in mine]
        other = other + [flip(v, "ep", core_bit) for v in other]
        mine = jnp.concatenate(mine, axis=0)
        other = jnp.concatenate(other, axis=0)
        body = mine[:, :half]
        full = jnp.where(
            my_x == 0,
            jnp.concatenate([body, other], axis=1),
            jnp.concatenate([other, body], axis=1),
        )
        return full, mine[:, half:]

    rows_own = to_group(rows_half)
    cot_own = to_group(cot_half)
    rows, meta = in_plane(rows_own)
    cot, _ = in_plane(cot_own)
    mine_lane = lane == my_member
    scale = jnp.sum(jnp.where(mine_lane, meta.astype(jnp.float32), 0.0), axis=1, keepdims=True)

    gate_cols, up_cols, down_part = w_gate[0], w_up[0], w_down[0]
    gate_pre = mm(rows, gate_cols, ((1,), (0,)))
    up_pre = mm(rows, up_cols, ((1,), (0,)))
    hidden_back = mm(cot, down_part, ((1,), (1,)))
    gate_sig = jax.nn.sigmoid(gate_pre)
    activated = gate_pre * gate_sig
    hidden = activated * up_pre
    route_part = jnp.sum(hidden * hidden_back, axis=1, keepdims=True)
    hidden_cot = scale * hidden_back
    up_cot = (hidden_cot * activated).astype(bf)
    gate_cot = (hidden_cot * up_pre * gate_sig * (1.0 + gate_pre * (1.0 - gate_sig))).astype(bf)
    weighted_hidden = (scale * hidden).astype(bf)
    route_lanes = jnp.where(mine_lane, route_part, 0.0).astype(bf)

    def back_piece(which):
        start = which * half
        g_part = lax.dynamic_slice_in_dim(gate_cols, start, half, 0)
        u_part = lax.dynamic_slice_in_dim(up_cols, start, half, 0)
        term = mm(gate_cot, g_part, ((1,), (1,))) + mm(up_cot, u_part, ((1,), (1,)))
        return jnp.concatenate([term.astype(bf), route_lanes], axis=1)

    slots = GROUPS * cap
    cut = slots // 2
    away = back_piece(1 - my_x)
    stay = back_piece(my_x)
    away_in = flip(away[2 * slots :], "ep", core_bit)
    stay_in = flip(stay[2 * slots :], "ep", core_bit)

    def chip_sum(here, there, start):
        return add(here[start : start + cut], there[start : start + cut])

    a_xo = flip(chip_sum(away, away_in, slots), "tp", 1)
    b_xy = flip(chip_sum(away, away_in, slots + cut), "ep", row_bit)
    a_x = flip(chip_sum(away, away_in, 0), "tp", 1)
    b_y = flip(chip_sum(stay, stay_in, slots + cut), "ep", row_bit)
    a_next = flip(add(chip_sum(stay, stay_in, slots), a_xo), "ep", row_bit)
    b_next = flip(add(chip_sum(away, away_in, cut), b_xy), "tp", 1)
    a_end = add(add(chip_sum(stay, stay_in, 0), a_x), a_next)
    b_end = add(add(chip_sum(stay, stay_in, cut), b_y), b_next)
    done = []
    for k in range(GROUPS):
        side = a_end if k < GROUPS // 2 else b_end
        at = (k % (GROUPS // 2)) * cap
        piece = side[at : at + cap]
        done.append(piece if k == 0 else flip(piece, "ep", k * members))
    landed = jnp.concatenate(done, axis=0)
    result = mm(pack, landed, ((0,), (0,)))
    token_grad = result[:, :half].astype(bf)
    tail = result[:, half:]
    route_grad = jnp.concatenate(
        [jnp.sum(jnp.where(p, tail, 0.0), axis=1, keepdims=True) for p in picks], axis=1
    ).astype(bf)

    grad_down = mm(weighted_hidden, cot, ((0,), (0,))).astype(bf)
    grad_gate = mm(rows, gate_cot, ((0,), (0,))).astype(bf)
    grad_up = mm(rows, up_cot, ((0,), (0,))).astype(bf)
    gate_square = jnp.sum(jnp.square(grad_gate.astype(jnp.float32)), axis=1)
    up_square = jnp.sum(jnp.square(grad_up.astype(jnp.float32)), axis=1)
    down_square = jnp.sum(jnp.square(grad_down.astype(jnp.float32)), axis=1)
    squares = jnp.stack([gate_square, up_square])
    squares = squares + flip(squares, "tp", 1)
    return (
        token_grad,
        route_grad,
        grad_gate[None],
        grad_up[None],
        grad_down[None],
        squares[0:1],
        squares[1:2],
        down_square[None],
    )


def solution(mesh):
    small = mesh.shape["ep"] == 4 * GROUPS and mesh.shape["tp"] == 2
    return jax.shard_map(
        in_groups if small else on_device,
        mesh=mesh,
        in_specs=(
            P("ep", None),
            P("ep", None),
            P("ep", None),
            P("ep", None),
            P("ep", None, "tp"),
            P("ep", None, "tp"),
            P("ep", "tp", None),
        ),
        out_specs=(
            P("ep", "tp"),
            P("ep", None),
            P("ep", None, "tp"),
            P("ep", None, "tp"),
            P("ep", "tp", None),
            P("ep", None),
            P("ep", None),
            P("ep", "tp"),
        ),
        check_vma=False,
    )
```

```python
import jax
import jax.numpy as jnp
from jax import lax
from jax.sharding import PartitionSpec as P

TOPK = 2


def on_device(tokens, expert_ids, route_weights, cotangent, w_gate, w_up, w_down):
    tok_rows, model_width = tokens.shape
    experts = lax.axis_size("ep")
    splits = lax.axis_size("tp")
    capacity = 2 * tok_rows * TOPK // experts
    slot_count = experts * capacity
    assigns = tok_rows * TOPK
    flat_ids = expert_ids.reshape(-1)
    onehot = (flat_ids[:, None] == jnp.arange(experts, dtype=jnp.int32)[None, :]).astype(
        jnp.float32
    )
    assign_order = jnp.arange(assigns, dtype=jnp.int32)
    earlier = (assign_order[:, None] > assign_order[None, :]).astype(jnp.float32)
    before = jnp.dot(earlier, onehot, precision=lax.Precision.HIGHEST)
    slot_rank = jnp.sum(before * onehot, axis=1).astype(jnp.int32)
    position = flat_ids * capacity + slot_rank
    slot_owner = jnp.full((slot_count,), tok_rows, jnp.int32).at[position].set(assign_order // TOPK)
    slot_scale = jnp.zeros((slot_count,), jnp.bfloat16).at[position].set(route_weights.reshape(-1))
    slice_width = model_width // splits
    slice_start = lax.axis_index("tp") * slice_width
    rows_slice = lax.dynamic_slice_in_dim(tokens, slice_start, slice_width, 1)
    cot_slice = lax.dynamic_slice_in_dim(cotangent, slice_start, slice_width, 1)
    rows_pad = jnp.concatenate([rows_slice, jnp.zeros((1, slice_width), jnp.bfloat16)], axis=0)
    cot_pad = jnp.concatenate([cot_slice, jnp.zeros((1, slice_width), jnp.bfloat16)], axis=0)
    outgoing = rows_pad[slot_owner]
    outgoing_cot = cot_pad[slot_owner]
    part_rows, part_cot, got_scale = (
        lax.all_to_all(outgoing, "ep", split_axis=0, concat_axis=0, tiled=True),
        lax.all_to_all(outgoing_cot, "ep", split_axis=0, concat_axis=0, tiled=True),
        lax.all_to_all(slot_scale, "ep", split_axis=0, concat_axis=0, tiled=True),
    )
    slot_rows, slot_cot = (
        lax.all_gather(part_rows, "tp", axis=1, tiled=True),
        lax.all_gather(part_cot, "tp", axis=1, tiled=True),
    )
    scale_col = got_scale.reshape(slot_count, 1).astype(jnp.float32)
    gate_cols = w_gate[0]
    up_cols = w_up[0]
    down_part = w_down[0]
    gate_pre = jnp.dot(slot_rows, gate_cols, preferred_element_type=jnp.float32)
    up_pre = jnp.dot(slot_rows, up_cols, preferred_element_type=jnp.float32)
    hidden_back = lax.dot_general(
        slot_cot, down_part, (((1,), (1,)), ((), ())), preferred_element_type=jnp.float32
    )
    gate_sig = jax.nn.sigmoid(gate_pre)
    activated = gate_pre * gate_sig
    hidden = activated * up_pre
    route_part = jnp.sum(hidden * hidden_back, axis=1)
    hidden_cot = scale_col * hidden_back
    up_cot = (hidden_cot * activated).astype(jnp.bfloat16)
    gate_cot = (hidden_cot * up_pre * gate_sig * (1.0 + gate_pre * (1.0 - gate_sig))).astype(
        jnp.bfloat16
    )
    weighted_hidden = (scale_col * hidden).astype(jnp.bfloat16)
    grad_down = lax.dot_general(
        weighted_hidden, slot_cot, (((0,), (0,)), ((), ())), preferred_element_type=jnp.float32
    ).astype(jnp.bfloat16)
    grad_gate = lax.dot_general(
        slot_rows, gate_cot, (((0,), (0,)), ((), ())), preferred_element_type=jnp.float32
    ).astype(jnp.bfloat16)
    grad_up = lax.dot_general(
        slot_rows, up_cot, (((0,), (0,)), ((), ())), preferred_element_type=jnp.float32
    ).astype(jnp.bfloat16)
    token_term = lax.dot_general(
        gate_cot, gate_cols, (((1,), (1,)), ((), ())), preferred_element_type=jnp.float32
    )
    token_term = token_term + lax.dot_general(
        up_cot, up_cols, (((1,), (1,)), ((), ())), preferred_element_type=jnp.float32
    )
    reduced = lax.psum_scatter(
        token_term.astype(jnp.bfloat16), "tp", scatter_dimension=1, tiled=True
    )
    gate_square = jnp.sum(jnp.square(grad_gate.astype(jnp.float32)), axis=1)
    up_square = jnp.sum(jnp.square(grad_up.astype(jnp.float32)), axis=1)
    down_square = jnp.sum(jnp.square(grad_down.astype(jnp.float32)), axis=1)
    route_total, gate_rows, up_rows = lax.psum((route_part, gate_square, up_square), "tp")
    back_rows, back_route = (
        lax.all_to_all(reduced, "ep", split_axis=0, concat_axis=0, tiled=True),
        lax.all_to_all(
            route_total.astype(jnp.bfloat16), "ep", split_axis=0, concat_axis=0, tiled=True
        ),
    )
    per_assign = back_rows[position].astype(jnp.float32).reshape(tok_rows, TOPK, -1)
    token_grad = jnp.sum(per_assign, axis=1).astype(jnp.bfloat16)
    route_grad = back_route[position].reshape(tok_rows, TOPK)
    return (
        token_grad,
        route_grad,
        grad_gate[None],
        grad_up[None],
        grad_down[None],
        gate_rows[None],
        up_rows[None],
        down_square[None],
    )

GROUPS = 4
LANES = 128


def flip(value, axis, bit):
    size = lax.axis_size(axis)
    return lax.ppermute(value, axis, [(i, i ^ bit) for i in range(size)])


def mm(a, b, dims):
    return lax.dot_general(a, b, (dims, ((), ())), preferred_element_type=jnp.float32)


def add(a, b):
    return (a.astype(jnp.float32) + b.astype(jnp.float32)).astype(jnp.bfloat16)


def in_groups(tokens, expert_ids, route_weights, cotangent, w_gate, w_up, w_down):
    tok_rows, width = tokens.shape
    experts = lax.axis_size("ep")
    splits = lax.axis_size("tp")
    members = experts // GROUPS
    cap = tok_rows * TOPK // GROUPS
    half = width // splits
    my_x = lax.axis_index("tp")
    my_ep = lax.axis_index("ep")
    my_group = my_ep // members
    my_member = my_ep % members
    core_bit, row_bit = 1, members // 2
    bf = jnp.bfloat16

    group = (expert_ids[:, 0] // members) ^ my_group
    member = expert_ids % members
    onehot = (group[:, None] == jnp.arange(GROUPS, dtype=jnp.int32)[None, :]).astype(bf)
    order = jnp.arange(tok_rows, dtype=jnp.int32)
    earlier = (order[:, None] > order[None, :]).astype(bf)
    before = mm(earlier, onehot, ((1,), (0,)))
    rank = jnp.sum(before * onehot.astype(jnp.float32), axis=1).astype(jnp.int32)
    slot = group * cap + rank
    pack = (jnp.arange(GROUPS * cap, dtype=jnp.int32)[:, None] == slot[None, :]).astype(bf)
    lane = jnp.arange(LANES, dtype=jnp.int32)[None, :]
    picks = [lane == member[:, k : k + 1] for k in range(TOPK)]
    weights = sum(
        jnp.where(picks[k], route_weights[:, k : k + 1].astype(jnp.float32), 0.0)
        for k in range(TOPK)
    ).astype(bf)
    rows_half = lax.dynamic_slice_in_dim(tokens, my_x * half, half, 1)
    cot_half = lax.dynamic_slice_in_dim(cotangent, my_x * half, half, 1)
    source = jnp.concatenate([rows_half, cot_half, weights], axis=1)

    own, other = {}, {}
    for k in (1, 2, 3, 0):
        unit = mm(pack[k * cap : (k + 1) * cap], source, ((1,), (0,))).astype(bf)
        if k:
            unit = flip(unit, "ep", k * members)
        over_x = flip(unit, "tp", 1)
        over_y = flip(unit, "ep", row_bit)
        diag = flip(over_y, "tp", 1) if k % 2 == 0 else flip(over_x, "ep", row_bit)
        own[k] = [unit, over_y], [flip(unit, "ep", core_bit), flip(over_y, "ep", core_bit)]
        other[k] = [over_x, diag], [flip(over_x, "ep", core_bit), flip(diag, "ep", core_bit)]

    chunks = ((0, 1), (2, 3))

    def stack(pieces, lo, hi):
        return jnp.concatenate(
            [p[:, lo:hi] for ch in chunks for c in range(2) for k in ch for p in pieces[k][c]],
            axis=0,
        )

    rows_s, rows_o = stack(own, 0, half), stack(other, 0, half)
    cot_s, cot_o = stack(own, half, 2 * half), stack(other, half, 2 * half)
    meta = stack(own, 2 * half, 2 * half + LANES)
    mine_lane = lane == my_member
    scale = jnp.sum(jnp.where(mine_lane, meta.astype(jnp.float32), 0.0), axis=1, keepdims=True)

    def halves(value, dim):
        return [
            lax.dynamic_slice_in_dim(value, which * half, half, dim)
            for which in (my_x, 1 - my_x)
        ]

    gate_s, gate_o = halves(w_gate[0], 0)
    up_s, up_o = halves(w_up[0], 0)
    down_s, down_o = halves(w_down[0], 1)
    last = ((1,), (0,))
    gate_pre = mm(rows_s, gate_s, last) + mm(rows_o, gate_o, last)
    up_pre = mm(rows_s, up_s, last) + mm(rows_o, up_o, last)
    hidden_back = mm(cot_s, down_s, ((1,), (1,))) + mm(cot_o, down_o, ((1,), (1,)))
    gate_sig = jax.nn.sigmoid(gate_pre)
    activated = gate_pre * gate_sig
    hidden = activated * up_pre
    route_part = jnp.sum(hidden * hidden_back, axis=1, keepdims=True)
    hidden_cot = scale * hidden_back
    up_cot = (hidden_cot * activated).astype(bf)
    gate_cot = (hidden_cot * up_pre * gate_sig * (1.0 + gate_pre * (1.0 - gate_sig))).astype(bf)
    weighted_hidden = (scale * hidden).astype(bf)
    route_lanes = jnp.where(mine_lane, route_part, 0.0).astype(bf)

    per_core = 4 * cap

    def term(at, g_part, u_part):
        value = mm(gate_cot[at : at + per_core], g_part, ((1,), (1,)))
        value = value + mm(up_cot[at : at + per_core], u_part, ((1,), (1,)))
        return jnp.concatenate([value.astype(bf), route_lanes[at : at + per_core]], axis=1)

    def leave(chunk):
        at = 2 * chunk * per_core
        away_in = flip(term(at + per_core, gate_o, up_o), "ep", core_bit)
        stay_in = flip(term(at + per_core, gate_s, up_s), "ep", core_bit)
        return term(at, gate_o, up_o), term(at, gate_s, up_s), away_in, stay_in

    def first_sends(away, stay, away_in, stay_in):
        away = add(away, away_in)
        stay = add(stay, stay_in)
        cuts = lambda v: [v[i * cap : (i + 1) * cap] for i in range(4)]
        return cuts(away), cuts(stay)

    def finish(away, stay):
        a_xo = flip(away[1], "tp", 1)
        b_xy = flip(away[3], "ep", row_bit)
        a_x = flip(away[0], "tp", 1)
        b_y = flip(stay[3], "ep", row_bit)
        a_next = flip(add(stay[1], a_xo), "ep", row_bit)
        b_next = flip(add(away[2], b_xy), "tp", 1)
        return add(add(stay[0], a_x), a_next), add(add(stay[2], b_y), b_next)

    far = leave(1)
    near = leave(0)
    wait_down = lax.optimization_barrier((weighted_hidden,) + near[:2])[0]
    far = first_sends(*far)
    wait_gate = lax.optimization_barrier((gate_cot, far))[0]
    near = first_sends(*near)
    wait_up = lax.optimization_barrier((up_cot, near))[0]
    unit2, unit3 = finish(*far)
    unit0, unit1 = finish(*near)
    landed = jnp.concatenate(
        [
            unit0,
            flip(unit1, "ep", members),
            flip(unit2, "ep", 2 * members),
            flip(unit3, "ep", 3 * members),
        ],
        axis=0,
    )
    result = mm(pack, landed, ((0,), (0,)))
    token_grad = result[:, :half].astype(bf)
    tail = result[:, half:]
    route_grad = jnp.concatenate(
        [jnp.sum(jnp.where(p, tail, 0.0), axis=1, keepdims=True) for p in picks], axis=1
    ).astype(bf)

    def ordered(mine, others, dim):
        return jnp.where(
            my_x == 0,
            jnp.concatenate([mine, others], axis=dim),
            jnp.concatenate([others, mine], axis=dim),
        )

    def square(value):
        return jnp.sum(jnp.square(value.astype(jnp.float32)), axis=1)

    first = ((0,), (0,))
    down_gs, down_go = mm(wait_down, cot_s, first).astype(bf), mm(wait_down, cot_o, first).astype(bf)
    gate_gs, gate_go = mm(rows_s, wait_gate, first).astype(bf), mm(rows_o, wait_gate, first).astype(bf)
    up_gs, up_go = mm(rows_s, wait_up, first).astype(bf), mm(rows_o, wait_up, first).astype(bf)
    down_square = square(down_gs) + square(down_go)
    squares = jnp.stack(
        [
            ordered(square(gate_gs), square(gate_go), 0),
            ordered(square(up_gs), square(up_go), 0),
        ]
    )
    squares = squares + flip(squares, "tp", 1)
    return (
        token_grad,
        route_grad,
        ordered(gate_gs, gate_go, 0)[None],
        ordered(up_gs, up_go, 0)[None],
        ordered(down_gs, down_go, 1)[None],
        squares[0:1],
        squares[1:2],
        down_square[None],
    )


def solution(mesh):
    small = mesh.shape["ep"] == 4 * GROUPS and mesh.shape["tp"] == 2
    return jax.shard_map(
        in_groups if small else on_device,
        mesh=mesh,
        in_specs=(
            P("ep", None),
            P("ep", None),
            P("ep", None),
            P("ep", None),
            P("ep", None, "tp"),
            P("ep", None, "tp"),
            P("ep", "tp", None),
        ),
        out_specs=(
            P("ep", "tp"),
            P("ep", None),
            P("ep", None, "tp"),
            P("ep", None, "tp"),
            P("ep", "tp", None),
            P("ep", None),
            P("ep", None),
            P("ep", "tp"),
        ),
        check_vma=False,
    )
```
